256 devices in a mesh: sp: 64 (over z, y, core), tp: 4 (over x).
Axes of the slice: x: 4, y: 4, z: 8, core: 2. Of those that a mesh axis runs over, the one named last changes fastest.
Arguments:
- stream: bfloat16 [32768, 2048], P('sp', 'tp'), may hold values from -6 to 6
- doc_ids: int32 [32768], P('sp'), may hold values from 0 to 15, never falling along the last dimension, each value on 1 to 16640 neighbouring positions
- norm_gain: float32 [2, 2048], replicated, may hold values from 0.1 to 1.9
- gate_proj: bfloat16 [2, 2048, 2048], P(None, 'sp', 'tp'), may hold values from -0.125 to 0.125
- input_gate: bfloat16 [2, 2048, 2048], P(None, 'sp', 'tp'), may hold values from -0.125 to 0.125
- value_proj: bfloat16 [2, 2048, 2048], P(None, 'sp', 'tp'), may hold values from -0.125 to 0.125
- taps: float32 [2, 3, 2048], P(None, None, 'tp'), may hold values from -3 to 3
- out_proj: bfloat16 [2, 2048, 2048], P(None, 'tp', 'sp'), may hold values from -0.125 to 0.125
Outputs:
- result: bfloat16 [32768, 2048], P('sp', 'tp')
The draws below stay inside these ranges and needn't reach their ends.
Inputs may be any that keep to these rules, and one draw needn't show every extreme that they name: `doc_ids`: document numbers never fall along the sequence; each document holds 1 to 16640 positions.
All inputs are finite; a program needn't handle non-finite values.
Results may differ from the reference program's by a relative error of at most 0.03.
Values may be sent and summed in bfloat16 or wider, within the bound.
No kernel may reach another device: no remote copies, remote signals or barrier semaphores. Data moves between devices by JAX's collectives and lax.ppermute only.
A program may use at most 64 MiB of HBM per device.

```python
import math
import jax
import jax.numpy as jnp
import numpy as np
from jax import lax

D = 2048
CW = 2048
LAYERS = 2
TOKENS = 32768
DOCS = 16
DOC_MOST = 16640
N_TP = 4


def steps_of(rng, dims, cuts, least, high):
    def one(dim, blocks):
        draws = jax.random.uniform(jax.random.fold_in(jax.random.fold_in(rng, 6), dim), (blocks,), jnp.float32, least / len(cuts), high / len(cuts))
        return jnp.repeat(jnp.exp(draws), dims[dim] // blocks).reshape((-1,) + (1,) * (len(dims) - dim - 1))

    loudness = one(*cuts[0])
    for cut in cuts[1:]:
        loudness = loudness * one(*cut)
    return loudness


def length_profile(amount, total, bound, lean):
    loads = [(1 << 20) // math.isqrt(grade ** lean) + 1 for grade in range(2, amount + 1)]
    surplus, holding = total - bound - (amount - 1), [1] * (amount - 1)
    while surplus > 0:
        candidates = [i for i in range(amount - 1) if holding[i] < bound]
        pool, left = sum([loads[i] for i in candidates]), surplus
        for i in candidates:
            addition = min(bound - holding[i], max(1, left * loads[i] // pool), surplus)
            holding[i] = holding[i] + addition
            surplus = surplus - addition
    return np.array([bound] + holding)


def ragged_sizes(own_key, amount, total, most, slope):
    if amount == 2:
        one = jax.random.randint(own_key, (), max(1, total - most), min(most, total - 1) + 1)
        return jnp.stack([one, total - one])
    sizes = jnp.asarray(length_profile(amount, total, most, slope), jnp.int32)
    pairs = (amount - 1) // 2
    source_of, taker = sizes[1:1 + 2 * pairs:2], sizes[2:2 + 2 * pairs:2]
    room = jnp.minimum(source_of - 1, most - taker)
    moved = jax.random.randint(jax.random.fold_in(own_key, 1), (pairs,), 0, 1 << 20) % (room + 1)
    sizes = sizes.at[1:1 + 2 * pairs:2].set(source_of - moved).at[2:2 + 2 * pairs:2].set(taker + moved)
    return sizes[jax.random.permutation(jax.random.fold_in(own_key, 2), amount)]


def noise(stream_key, shape, spread, limit, split=(), kind=jnp.bfloat16):
    entries = spread * jax.random.normal(stream_key, shape, jnp.float32)
    if split:
        entries = entries * steps_of(stream_key, shape, split, -0.22, 0.18)
    return jnp.clip(entries, -limit, limit).astype(kind)


def setup_inputs(seed: int = 0) -> dict:
    key_of = jax.random.split(jax.random.key(seed), 9)
    return {
        "stream": noise(key_of[0], (TOKENS, D), 1.0, 6.0, ((0, 64), (1, 4))),
        "doc_ids": jnp.searchsorted(jnp.cumsum(ragged_sizes(key_of[1], DOCS, TOKENS, DOC_MOST, 1)), jnp.arange(TOKENS), side="right").astype(jnp.int32),
        "norm_gain": jnp.clip(1.0 + 0.18 * jax.random.normal(key_of[2], (LAYERS, D), jnp.float32), 0.1, 1.9),
        "gate_proj": noise(key_of[3], (LAYERS, D, CW), D ** -0.5, 0.125, ((1, 64), (2, 4))),
        "input_gate": noise(key_of[4], (LAYERS, D, CW), D ** -0.5, 0.125, ((1, 64), (2, 4))),
        "value_proj": noise(key_of[5], (LAYERS, D, CW), D ** -0.5, 0.125, ((1, 64), (2, 4))),
        "taps": noise(key_of[6], (LAYERS, 3, CW), 0.5, 3.0, ((2, 4),), jnp.float32),
        "out_proj": noise(key_of[7], (LAYERS, CW, D), CW ** -0.5, 0.125, ((1, 4), (2, 64))),
    }


epsilon = 1e-06

def reference(stream, doc_ids, norm_gain, gate_proj, input_gate, value_proj, taps, out_proj):
    block = CW // N_TP
    current = stream
    for layer_index in range(LAYERS):
        widened = current.astype(jnp.float32)
        scale = lax.rsqrt(lax.optimization_barrier(jnp.mean(widened * widened, axis=-1, keepdims=True)) + epsilon)
        normed = (widened * scale * norm_gain[layer_index]).astype(jnp.bfloat16)
        gate_b = jnp.dot(normed, gate_proj[layer_index], preferred_element_type=jnp.float32).astype(jnp.bfloat16)
        gate_c = jnp.dot(normed, input_gate[layer_index], preferred_element_type=jnp.float32).astype(jnp.bfloat16)
        values = jnp.dot(normed, value_proj[layer_index], preferred_element_type=jnp.float32).astype(jnp.bfloat16)
        mixed_in = (gate_c.astype(jnp.float32) * values.astype(jnp.float32)).astype(jnp.bfloat16)
        mixed_wide = mixed_in.astype(jnp.float32)
        zero_row = jnp.zeros((1, CW), jnp.float32)
        before = jnp.concatenate([zero_row, mixed_wide[:-1]], axis=0)
        after = jnp.concatenate([mixed_wide[1:], zero_row], axis=0)
        same_doc = doc_ids[1:] == doc_ids[:-1]
        false_edge = jnp.zeros((1,), bool)
        same_prev = jnp.concatenate([false_edge, same_doc])[:, None]
        same_next = jnp.concatenate([same_doc, false_edge])[:, None]
        kernel_taps = taps[layer_index]
        convolved = jnp.where(same_prev, kernel_taps[0] * before, 0.0) + kernel_taps[1] * mixed_wide + jnp.where(same_next, kernel_taps[2] * after, 0.0)
        gated = (gate_b.astype(jnp.float32) * convolved).astype(jnp.bfloat16)
        total = jnp.zeros((TOKENS, D), jnp.float32)
        for block_index in range(N_TP):
            lower = block_index * block
            partial_value = jnp.dot(gated[:, lower:lower + block], out_proj[layer_index][lower:lower + block], preferred_element_type=jnp.float32).astype(jnp.bfloat16)
            total = total + partial_value.astype(jnp.float32)
        current = (current.astype(jnp.float32) + total).astype(jnp.bfloat16)
    return current
```

```python
import functools

import jax
import jax.numpy as jnp
from jax import lax
from jax.experimental import pallas as pl
from jax.experimental.pallas import tpu as pltpu
from jax.sharding import Mesh
from jax.sharding import PartitionSpec as P

epsilon = 1e-06
NZ, NY, NC, NX = 8, 4, 2, 4
SP = ("z", "y", "c")
HALO = 8


def shifted(value, axis, step):
    size = lax.axis_size(axis)
    return lax.ppermute(value, axis, [(i, (i + step) % size) for i in range(size)])


def partner(value):
    return lax.ppermute(value, "c", [(0, 1), (1, 0)])


def with_edges(value, fill):
    size = lax.axis_size(SP)
    me = lax.axis_index(SP)
    before = lax.ppermute(value[-HALO:], SP, [(i, i + 1) for i in range(size - 1)])
    after = lax.ppermute(value[:HALO], SP, [(i + 1, i) for i in range(size - 1)])
    if fill is not None:
        before = jnp.where(me == 0, fill, before)
        after = jnp.where(me == size - 1, fill, after)
    return jnp.concatenate([before, value, after], axis=0)


Y_OFF = (0, -1, 1, 2)
Z_OFF = (0, -1, 1, -2, 2, -3, 3, 4)


def gather_a(a):
    ay = jnp.stack([a, shifted(a, "y", 1), shifted(a, "y", -1), shifted(a, "y", 2)])
    pieces = [(0, 0, ay)]
    right, left = ay, ay
    for step in (1, 2, 3):
        right, left = shifted(right, "z", 1), shifted(left, "z", -1)
        pieces += [(-step, 0, right), (step, 0, left)]
    pieces += [(4, 0, shifted(right[:2], "z", 1)), (4, 2, shifted(left[2:], "z", -1))]
    return pieces


def gather_b(b):
    bz = jnp.stack([b if off == 0 else shifted(b, "z", -off) for off in Z_OFF])
    right, left = shifted(bz, "y", 1), shifted(bz, "y", -1)
    opposite = [(2, 0, shifted(right[:4], "y", 1)), (2, 4, shifted(left[4:], "y", -1))]
    return [(0, 0, bz), (-1, 0, right), (1, 0, left)] + opposite


def gather_x(top, bottom):
    left_top, right_bottom = shifted(top, "x", 1), shifted(bottom, "x", -1)
    left_bottom, right_top = shifted(bottom, "x", 1), shifted(top, "x", -1)
    far_top, far_bottom = shifted(left_top, "x", 1), shifted(right_bottom, "x", -1)
    return (top, left_top, right_top, far_top), (bottom, left_bottom, right_bottom, far_bottom)


def wide(value):
    return value.astype(jnp.float32)


def scatter_x(stream, parts):
    top, bottom = stream
    (self_top, right_top, left_top, far_top), (self_bottom, right_bottom, left_bottom, far_bottom) = parts
    got_top, got_bottom = shifted(far_top, "x", 1), shifted(far_bottom, "x", -1)
    from_left_bottom, from_right_top = shifted(right_bottom, "x", 1), shifted(left_top, "x", -1)
    joined_top = (wide(right_top) + wide(got_top)).astype(jnp.bfloat16)
    joined_bottom = (wide(left_bottom) + wide(got_bottom)).astype(jnp.bfloat16)
    from_left_top, from_right_bottom = shifted(joined_top, "x", 1), shifted(joined_bottom, "x", -1)
    top = wide(top) + (wide(self_top) + wide(from_left_top) + wide(from_right_top))
    bottom = wide(bottom) + (wide(self_bottom) + wide(from_left_bottom) + wide(from_right_bottom))
    return top.astype(jnp.bfloat16), bottom.astype(jnp.bfloat16)


def layer_kernel(shape_of, *refs):
    n_a, n_b, a_meta, b_meta = shape_of
    tops, refs = refs[:4], refs[4:]
    bottoms, refs = refs[:4], refs[4:]
    (gain, same, taps), refs = refs[:3], refs[3:]
    own_a, refs = refs[:n_a], refs[n_a:]
    own_b, refs = refs[:n_b], refs[n_b:]
    other_a, refs = refs[:n_a], refs[n_a:]
    other_b, refs = refs[:n_b], refs[n_b:]
    out_tops, refs = refs[:4], refs[4:]
    out_bottoms, refs = refs[:4], refs[4:]
    weights, normed, gated, sems = refs
    x, y, z, c = (lax.axis_index(name) for name in ("x", "y", "z", "c"))
    rows_top = tops[0].shape[0]

    def place(mat, z_off, y_off):
        row = lax.rem(z + z_off + NZ, NZ) * 256 + lax.rem(y + y_off + NY, NY) * 64
        return weights.at[mat, pl.ds(pl.multiple_of(row, 64), 64)]

    for core, pieces_a, pieces_b in ((c, own_a, own_b), (1 - c, other_a, other_b)):
        for (z_off, first, count), piece in zip(a_meta, pieces_a):
            for k in range(count):
                pltpu.make_async_copy(
                    piece.at[k], place(2 * core, z_off, Y_OFF[first + k]), sems.at[2 * core]
                ).start()
        for (y_off, first, count), piece in zip(b_meta, pieces_b):
            for k in range(count):
                pltpu.make_async_copy(
                    piece.at[k], place(2 * core + 1, Z_OFF[first + k], y_off), sems.at[2 * core + 1]
                ).start()

    blocks = [lax.rem(x + off + NX, NX) for off in (0, -1, 1, 2)]
    gains = [gain[pl.ds(block, 1), :] for block in blocks]
    step = 16
    for parts, base in ((tops, 0), (bottoms, rows_top)):

        def normalise(i, carry, parts=parts, base=base):
            rows = pl.ds(pl.multiple_of(i * step, step), step)
            values = [part[rows, :].astype(jnp.float32) for part in parts]
            total = sum(jnp.sum(v * v, axis=1, keepdims=True) for v in values)
            scale = lax.rsqrt(total * (1.0 / (512 * NX)) + epsilon)
            there = pl.ds(pl.multiple_of(base + i * step, step), step)
            for block, own_gain, v in zip(blocks, gains, values):
                columns = pl.ds(pl.multiple_of(block * 512, 512), 512)
                normed[there, columns] = (v * scale * own_gain).astype(jnp.bfloat16)
            return carry

        lax.fori_loop(0, parts[0].shape[0] // step, normalise, 0)

    for mat in range(3):
        pltpu.make_async_copy(weights.at[mat], weights.at[mat], sems.at[mat]).wait()

    rows_all = normed.shape[0]
    same_before, same_after = same[:, 0:1] > 0.5, same[:, 1:2] > 0.5

    def mix(n, carry):
        columns = pl.ds(pl.multiple_of(n * 256, 256), 256)

        def project(mat):
            value = jnp.dot(normed[...], weights[mat, :, columns], preferred_element_type=jnp.float32)
            return value.astype(jnp.bfloat16).astype(jnp.float32)

        mixed = (project(0) * project(1)).astype(jnp.bfloat16).astype(jnp.float32)
        before = pltpu.roll(mixed, 1, 0)
        after = pltpu.roll(mixed, rows_all - 1, 0)
        convolved = (
            jnp.where(same_before, taps[0:1, columns] * before, 0.0)
            + taps[1:2, columns] * mixed
            + jnp.where(same_after, taps[2:3, columns] * after, 0.0)
        )
        gated[:, columns] = (project(2) * convolved).astype(jnp.bfloat16)
        return carry

    lax.fori_loop(0, 2, mix, 0)
    pltpu.make_async_copy(weights.at[3], weights.at[3], sems.at[3]).wait()

    for off, top, bottom in zip((0, 1, -1, 2), out_tops, out_bottoms):
        block = lax.rem(x + off + NX, NX)

        def project_out(n, carry, block=block, top=top, bottom=bottom):
            rows = pl.ds(pl.multiple_of(block * 512 + n * 256, 256), 256)
            value = lax.dot_general(
                gated[...], weights[3, rows, :], (((1,), (1,)), ((), ())), preferred_element_type=jnp.float32
            ).astype(jnp.bfloat16)
            columns = pl.ds(pl.multiple_of(n * 256, 256), 256)
            top[:, columns] = value[:rows_top]
            bottom[:, columns] = value[rows_top:]
            return carry

        lax.fori_loop(0, 2, project_out, 0)


def layer(tops, bottoms, gain, same, taps, own_a, own_b, other_a, other_b):
    rows_top, rows_bottom = tops[0].shape[0], bottoms[0].shape[0]
    rows = rows_top + rows_bottom
    meta = (
        len(own_a),
        len(own_b),
        tuple((off, first, p.shape[0]) for off, first, p in own_a),
        tuple((off, first, p.shape[0]) for off, first, p in own_b),
    )
    pieces = [p for group in (own_a, own_b, other_a, other_b) for _, _, p in group]
    vmem, anywhere = pl.BlockSpec(memory_space=pltpu.VMEM), pl.BlockSpec(memory_space=pl.ANY)
    shapes = [jax.ShapeDtypeStruct((n, 512), jnp.bfloat16) for n in (rows_top,) * 4 + (rows_bottom,) * 4]
    outs = pl.pallas_call(
        functools.partial(layer_kernel, meta),
        out_shape=shapes,
        in_specs=[vmem] * 11 + [anywhere] * len(pieces),
        out_specs=[vmem] * 8,
        scratch_shapes=[
            pltpu.VMEM((4, 2048, 512), jnp.bfloat16),
            pltpu.VMEM((rows, 2048), jnp.bfloat16),
            pltpu.VMEM((rows, 512), jnp.bfloat16),
            pltpu.SemaphoreType.DMA((4,)),
        ],
        compiler_params=pltpu.CompilerParams(vmem_limit_bytes=32 * 1024 * 1024),
        cost_estimate=pl.CostEstimate(flops=2 * rows * 2048 * 2048, bytes_accessed=16 << 20, transcendentals=rows),
    )(*tops, *bottoms, gain, same, taps, *pieces)
    return outs[:4], outs[4:]


def per_device(stream, doc_ids, norm_gain, gate_proj, input_gate, value_proj, taps, out_proj):
    layers = gate_proj.shape[0]
    c = lax.axis_index("c")
    mats = jnp.stack([input_gate, value_proj, gate_proj, jnp.swapaxes(out_proj, 1, 2)], axis=1)
    keep = lax.dynamic_slice_in_dim(mats, 2 * c, 2, axis=1)
    give = lax.dynamic_slice_in_dim(mats, 2 * (1 - c), 2, axis=1)
    took = partner(give)
    mine = jnp.concatenate([jnp.where(c == 0, keep, took), jnp.where(c == 0, took, keep)], axis=2)

    whole = with_edges(stream, None)
    docs = with_edges(doc_ids, -1)
    rows = whole.shape[0]
    rows_top = (rows // 32 + 1) * 16
    current = whole[:rows_top], whole[rows_top:]
    equal = (docs[1:] == docs[:-1]).astype(jnp.float32)
    none = jnp.zeros((1,), jnp.float32)
    same = jnp.stack([jnp.concatenate([none, equal]), jnp.concatenate([equal, none])], axis=1)

    weights = []
    for index in range(layers):
        own_a, own_b = gather_a(mine[index, 0]), gather_b(mine[index, 1])
        other_a = [(off, first, partner(p)) for off, first, p in own_a]
        other_b = [(off, first, partner(p)) for off, first, p in own_b]
        weights.append((own_a, own_b, other_a, other_b))

    for index in range(layers):
        tops, bottoms = gather_x(*current)
        parts = layer(tops, bottoms, norm_gain[index].reshape(NX, 512), same, taps[index], *weights[index])
        current = scatter_x(current, parts)
    return jnp.concatenate(current, axis=0)[HALO:-HALO]


def solution(mesh):
    split = Mesh(mesh.devices.reshape(NZ, NY, NC, NX), ("z", "y", "c", "x"))
    in_specs = (
        P(SP, "x"),
        P(SP),
        P(),
        P(None, SP, "x"),
        P(None, SP, "x"),
        P(None, SP, "x"),
        P(None, None, "x"),
        P(None, "x", SP),
    )
    return jax.shard_map(
        per_device, mesh=split, in_specs=in_specs, out_specs=P(SP, "x"), check_vma=False
    )
```

```python
import functools

import jax
import jax.numpy as jnp
from jax import lax
from jax.experimental import pallas as pl
from jax.experimental.pallas import tpu as pltpu
from jax.sharding import Mesh
from jax.sharding import PartitionSpec as P

epsilon = 1e-06
NZ, NY, NC, NX = 8, 4, 2, 4
SP = ("z", "y", "c")
HALO = 8


def shifted(value, axis, step):
    size = lax.axis_size(axis)
    return lax.ppermute(value, axis, [(i, (i + step) % size) for i in range(size)])


def partner(value):
    return lax.ppermute(value, "c", [(0, 1), (1, 0)])


def onward(value, axis):
    size = lax.axis_size(axis)
    pairs = [(2 * i, 2 * ((i + 1) % size)) for i in range(size)]
    pairs += [(2 * i + 1, 2 * ((i - 1) % size) + 1) for i in range(size)]
    return lax.ppermute(value, (axis, "c"), pairs)


def with_edges(value):
    size = lax.axis_size(SP)
    before = lax.ppermute(value[-HALO:], SP, [(i, i + 1) for i in range(size - 1)])
    after = lax.ppermute(value[:HALO], SP, [(i + 1, i) for i in range(size - 1)])
    return jnp.concatenate([before, value, after], axis=0)


def half(units, c):
    count = units.shape[0] // 2
    return lax.dynamic_slice_in_dim(units, c * count, count, axis=0)


def with_partner(units):
    return jnp.concatenate([partner(units), units], axis=0)


def gather_weights(first, second, c):
    own = first[:2]
    near = onward(own, "y")
    opposite = onward(half(near, c), "y")
    mixed = jnp.concatenate([half(own, c), near, opposite], axis=0)
    around = with_partner(mixed)
    one = onward(around, "z")
    two = onward(one, "z")
    three = onward(two, "z")
    four = onward(three[4:], "z")
    moved = [one, two, three, four]
    group_a = [around] + moved + [partner(v) for v in moved]
    own = jnp.concatenate([first[2:3], second[:2], first[3:4], second[2:]], axis=0)
    steps = [half(own, c)]
    got = own
    for _ in range(3):
        got = onward(got, "z")
        steps.append(got)
    steps.append(onward(half(got, c), "z"))

    def joined(pick):
        parts = []
        for step in steps:
            for k in range(0, step.shape[0], 3):
                parts.append(step[k : k + 1] if pick == 0 else step[k + 1 : k + 3])
        return jnp.concatenate(parts, axis=0)

    groups = []
    for pick in (0, 1):
        around = with_partner(joined(pick))
        near = onward(around, "y")
        opposite = onward(near[near.shape[0] // 2 :], "y")
        groups.append([around, near, opposite, partner(near), partner(opposite)])
    return group_a, groups[0], groups[1]


def units_a(c, s):
    def mixed(c, s):
        return [(c, 0), (0, s), (1, s), (c, 2)]

    def around(c, s):
        return mixed(1 - c, -s) + mixed(c, s)

    def moved(c, s):
        full = [[(m, k * s, y) for m, y in around(c, s)] for k in (1, 2, 3)]
        return full + [[(m, 4, y) for m, y in mixed(c, s)]]

    return [[(m, 0, y) for m, y in around(c, s)]] + moved(c, s) + moved(1 - c, -s)


def units_b(c, s, base, count):
    def side(c, s):
        own = [(base + c * count + i, 0) for i in range(count)]
        full = [(base + i, k * s) for k in (1, 2, 3) for i in range(2 * count)]
        return own + full + [(base + c * count + i, 4) for i in range(count)]

    def around(c, s):
        return side(1 - c, -s) + side(c, s)

    def moved(c, s):
        return [[(m, z, s) for m, z in around(c, s)], [(m, z, 2) for m, z in side(c, s)]]

    return [[(m, z, 0) for m, z in around(c, s)]] + moved(c, s) + moved(1 - c, -s)


def gather_x(rows, top):
    left, right = shifted(rows, "x", 1), shifted(rows, "x", -1)
    return rows, left, right, shifted(left[:top], "x", 1), shifted(right[top:], "x", -1)


def wide(value):
    return value.astype(jnp.float32)


def scatter_x(rows, parts, top):
    own, right, left, far_top, far_bottom = parts
    got_top, got_bottom = shifted(far_top, "x", 1), shifted(far_bottom, "x", -1)
    right_top = (wide(right[:top]) + wide(got_top)).astype(jnp.bfloat16)
    left_bottom = (wide(left[top:]) + wide(got_bottom)).astype(jnp.bfloat16)
    from_left = shifted(jnp.concatenate([right_top, right[top:]], axis=0), "x", 1)
    from_right = shifted(jnp.concatenate([left[:top], left_bottom], axis=0), "x", -1)
    return (wide(rows) + (wide(own) + wide(from_left) + wide(from_right))).astype(jnp.bfloat16)


def layer_kernel(tables, *refs):
    (own, left, right, far_top, far_bottom, gain, same, taps), refs = refs[:8], refs[8:]
    n_pieces = len(refs) - 5 - 4
    pieces, refs = refs[:n_pieces], refs[n_pieces:]
    (out_own, out_right, out_left, out_far_top, out_far_bottom), refs = refs[:5], refs[5:]
    weights, normed, gated, sems = refs
    x, y, z, c = (lax.axis_index(name) for name in ("x", "y", "z", "c"))
    rows_top = far_top.shape[0]

    places = tables(c, 2 * c - 1)
    for piece, units in zip(pieces, places):
        for k, (mat, z_off, y_off) in enumerate(units):
            row = lax.rem(z + z_off + NZ, NZ) * 256 + lax.rem(y + y_off + NY, NY) * 64
            pltpu.make_async_copy(
                piece.at[k], weights.at[mat, pl.ds(pl.multiple_of(row, 64), 64)], sems.at[mat]
            ).start()

    blocks = [lax.rem(x + off + NX, NX) for off in (0, -1, 1, 2)]
    gains = [gain[pl.ds(block, 1), :] for block in blocks]
    step = 16
    for far, base in ((far_top, 0), (far_bottom, rows_top)):

        def normalise(i, carry, far=far, base=base):
            there = pl.ds(pl.multiple_of(base + i * step, step), step)
            values = [part[there, :].astype(jnp.float32) for part in (own, left, right)]
            values.append(far[pl.ds(pl.multiple_of(i * step, step), step), :].astype(jnp.float32))
            total = sum(jnp.sum(v * v, axis=1, keepdims=True) for v in values)
            scale = lax.rsqrt(total * (1.0 / (512 * NX)) + epsilon)
            for block, own_gain, v in zip(blocks, gains, values):
                columns = pl.ds(pl.multiple_of(block * 512, 512), 512)
                normed[there, columns] = (v * scale * own_gain).astype(jnp.bfloat16)
            return carry

        lax.fori_loop(0, far.shape[0] // step, normalise, 0)

    for mat in range(3):
        pltpu.make_async_copy(weights.at[mat], weights.at[mat], sems.at[mat]).wait()

    rows_all = normed.shape[0]
    same_before, same_after = same[:, 0:1] > 0.5, same[:, 1:2] > 0.5

    def mix(n, carry):
        columns = pl.ds(pl.multiple_of(n * 256, 256), 256)

        def project(mat):
            value = jnp.dot(normed[...], weights[mat, :, columns], preferred_element_type=jnp.float32)
            return value.astype(jnp.bfloat16).astype(jnp.float32)

        mixed = (project(0) * project(1)).astype(jnp.bfloat16).astype(jnp.float32)
        before = pltpu.roll(mixed, 1, 0)
        after = pltpu.roll(mixed, rows_all - 1, 0)
        convolved = (
            jnp.where(same_before, taps[0:1, columns] * before, 0.0)
            + taps[1:2, columns] * mixed
            + jnp.where(same_after, taps[2:3, columns] * after, 0.0)
        )
        gated[:, columns] = (project(2) * convolved).astype(jnp.bfloat16)
        return carry

    lax.fori_loop(0, 2, mix, 0)
    pltpu.make_async_copy(weights.at[3], weights.at[3], sems.at[3]).wait()

    for off, outs in ((2, (out_far_top, out_far_bottom)), (1, (out_right,)), (-1, (out_left,)), (0, (out_own,))):
        block = lax.rem(x + off + NX, NX)

        def project_out(n, carry, block=block, outs=outs):
            rows = pl.ds(pl.multiple_of(block * 512 + n * 256, 256), 256)
            value = lax.dot_general(
                gated[...], weights[3, rows, :], (((1,), (1,)), ((), ())), preferred_element_type=jnp.float32
            ).astype(jnp.bfloat16)
            columns = pl.ds(pl.multiple_of(n * 256, 256), 256)
            if len(outs) == 2:
                outs[0][:, columns] = value[:rows_top]
                outs[1][:, columns] = value[rows_top:]
            else:
                outs[0][:, columns] = value
            return carry

        lax.fori_loop(0, 2, project_out, 0)


def layer(parts, gain, same, taps, pieces, tables):
    rows, rows_top = parts[0].shape[0], parts[3].shape[0]
    vmem, hbm = pl.BlockSpec(memory_space=pltpu.VMEM), pl.BlockSpec(memory_space=pltpu.HBM)
    counts = (rows, rows, rows, rows_top, rows - rows_top)
    return pl.pallas_call(
        functools.partial(layer_kernel, tables),
        out_shape=[jax.ShapeDtypeStruct((n, 512), jnp.bfloat16) for n in counts],
        in_specs=[vmem] * 8 + [hbm] * len(pieces),
        out_specs=[vmem] * 5,
        scratch_shapes=[
            pltpu.VMEM((4, 2048, 512), jnp.bfloat16),
            pltpu.VMEM((rows, 2048), jnp.bfloat16),
            pltpu.VMEM((rows, 512), jnp.bfloat16),
            pltpu.SemaphoreType.DMA((4,)),
        ],
        compiler_params=pltpu.CompilerParams(vmem_limit_bytes=32 * 1024 * 1024),
        cost_estimate=pl.CostEstimate(flops=2 * rows * 2048 * 2048, bytes_accessed=16 << 20, transcendentals=rows),
    )(*parts, gain, same, taps, *pieces)


def per_device(stream, doc_ids, norm_gain, gate_proj, input_gate, value_proj, taps, out_proj):
    c = lax.axis_index("c")
    mats = jnp.stack([input_gate, value_proj, gate_proj, jnp.swapaxes(out_proj, 1, 2)], axis=1)
    took = partner(mats)
    chip = jnp.concatenate([jnp.where(c == 0, mats, took), jnp.where(c == 0, took, mats)], axis=2)
    group_a, group_b, group_second = gather_weights(chip[0], chip[1], c)

    ids = jnp.broadcast_to(doc_ids.astype(jnp.bfloat16)[:, None], (doc_ids.shape[0], 128))
    wider = with_edges(jnp.concatenate([stream, ids], axis=1))
    current = wider[:, :512]
    me, length = lax.axis_index(SP), doc_ids.shape[0]
    docs = wider[:, 512].astype(jnp.float32)
    place = lax.broadcasted_iota(jnp.int32, (length + 2 * HALO,), 0) + me * length
    docs = jnp.where((place < HALO) | (place >= lax.axis_size(SP) * length + HALO), -1.0, docs)
    equal = (docs[1:] == docs[:-1]).astype(jnp.float32)
    none = jnp.zeros((1,), jnp.float32)
    same = jnp.stack([jnp.concatenate([none, equal]), jnp.concatenate([equal, none])], axis=1)
    top = (current.shape[0] // 32 + 1) * 16

    def tables_first(c, s):
        return units_a(c, s) + units_b(c, s, 2, 1)

    def tables_second(c, s):
        return units_b(c, s, 0, 2)

    plans = ((group_a + group_b, tables_first), (group_second, tables_second))
    for index, (pieces, tables) in enumerate(plans):
        parts = gather_x(current, top)
        outs = layer(parts, norm_gain[index].reshape(NX, 512), same, taps[index], pieces, tables)
        current = scatter_x(current, outs, top)
    return current[HALO:-HALO]


def solution(mesh):
    split = Mesh(mesh.devices.reshape(NZ, NY, NC, NX), ("z", "y", "c", "x"))
    in_specs = (
        P(SP, "x"),
        P(SP),
        P(),
        P(None, SP, "x"),
        P(None, SP, "x"),
        P(None, SP, "x"),
        P(None, None, "x"),
        P(None, "x", SP),
    )
    return jax.shard_map(
        per_device, mesh=split, in_specs=in_specs, out_specs=P(SP, "x"), check_vma=False
    )
```

```python
import functools

import jax
import jax.numpy as jnp
from jax import lax
from jax.experimental import pallas as pl
from jax.experimental.pallas import tpu as pltpu
from jax.sharding import Mesh
from jax.sharding import PartitionSpec as P

epsilon = 1e-06
NZ, NY, NC, NX = 8, 4, 2, 4
SP = ("z", "y", "c")
HALO = 8


def shifted(value, axis, step):
    size = lax.axis_size(axis)
    return lax.ppermute(value, axis, [(i, (i + step) % size) for i in range(size)])


def partner(value):
    return lax.ppermute(value, "c", [(0, 1), (1, 0)])


def onward(value, axis, step=1):
    size = lax.axis_size(axis)
    pairs = [(2 * i, 2 * ((i + step) % size)) for i in range(size)]
    pairs += [(2 * i + 1, 2 * ((i - step) % size) + 1) for i in range(size)]
    return lax.ppermute(value, (axis, "c"), pairs)


def with_edges(value):
    size = lax.axis_size(SP)
    before = lax.ppermute(value[-HALO:], SP, [(i, i + 1) for i in range(size - 1)])
    after = lax.ppermute(value[:HALO], SP, [(i + 1, i) for i in range(size - 1)])
    return jnp.concatenate([before, value, after], axis=0)


def half(units, c):
    count = units.shape[0] // 2
    return lax.dynamic_slice_in_dim(units, c * count, count, axis=0)


def gather_weights(chip, c):
    own = chip[:2]
    mixed = jnp.concatenate([half(own, c), onward(own, "y"), onward(half(own, c), "y", 2)], axis=0)
    mine, others = mixed, partner(mixed)
    pieces = [mine, others]
    moved = []
    for k in range(1, 4):
        with jax.named_scope(f"a_z{k}"):
            mine, others = onward(mine, "z"), onward(others, "z")
        moved += [mine, others]
    with jax.named_scope("a_z4"):
        moved.append(onward(mine, "z"))
    pieces += moved + [partner(v) for v in moved]
    own = chip[2:]
    one, two = onward(own, "z"), onward(own, "z", 2)
    far = onward(jnp.concatenate([one, half(two, c)], axis=0), "z", 2)
    side = jnp.concatenate([half(own, c), one, two, far], axis=0)
    others = partner(side)
    near = onward(side, "y")
    moved = [near, onward(others, "y"), onward(near, "y")]
    pieces += [side, others] + moved + [partner(v) for v in moved]
    return pieces


def units_of(c, s):
    def mixed(c, s):
        return [(c, 0), (0, s), (1, s), (c, 2)]

    def moved_a(c, s):
        near = [mixed(c, s), mixed(1 - c, -s)]
        full = [[(m, k * s, y) for m, y in units] for k in (1, 2, 3) for units in near]
        return full + [[(m, 4, y) for m, y in mixed(c, s)]]

    def side(c, s):
        return [(2 + c, 0)] + [(m, k * s) for k in (1, 2, 3) for m in (2, 3)] + [(2 + c, 4)]

    def moved_b(c, s):
        blocks = [(side(c, s), s), (side(1 - c, -s), s), (side(c, s), 2)]
        return [[(m, z, y) for m, z in units] for units, y in blocks]

    here_a = [[(m, 0, y) for m, y in units] for units in (mixed(c, s), mixed(1 - c, -s))]
    here_b = [[(m, z, 0) for m, z in units] for units in (side(c, s), side(1 - c, -s))]
    return here_a + moved_a(c, s) + moved_a(1 - c, -s) + here_b + moved_b(c, s) + moved_b(1 - c, -s)


def gather_x(rows, way):
    left, right = shifted(rows, "x", 1), shifted(rows, "x", -1)
    return rows, left, right, shifted(left if way == 1 else right, "x", way)


def wide(value):
    return value.astype(jnp.float32)


def scatter_x(rows, parts, way):
    own, right, left, far = parts
    got = wide(shifted(far, "x", way))
    if way == 1:
        right = (wide(right) + got).astype(jnp.bfloat16)
    else:
        left = (wide(left) + got).astype(jnp.bfloat16)
    from_left, from_right = shifted(right, "x", 1), shifted(left, "x", -1)
    return (wide(rows) + (wide(own) + wide(from_left) + wide(from_right))).astype(jnp.bfloat16)


def layer_kernel(segments, n_sources, n_pieces, first, *refs):
    sources, refs = refs[:n_sources], refs[n_sources:]
    (gain, same, taps), refs = refs[:3], refs[3:]
    pieces, refs = refs[:n_pieces], refs[n_pieces:]
    outs, (weights, normed, gated, sems) = refs[:4], refs[4:]
    x, y, z, c = (lax.axis_index(name) for name in ("x", "y", "z", "c"))

    def whole(mat):
        return pltpu.make_async_copy(pieces[0].at[mat], weights.at[mat], sems.at[mat])

    if n_pieces == 1:
        for mat in range(4):
            whole(mat).start()

    blocks = [lax.rem(x + off + NX, NX) for off in (0, -1, 1, 2)]
    gains = [gain[pl.ds(block, 1), :] for block in blocks]
    step = 16
    base = 0
    for count, places in segments:

        def normalise(i, carry, base=base, places=places):
            there = pl.ds(pl.multiple_of(base + i * step, step), step)
            values = [
                sources[k][pl.ds(pl.multiple_of(offset + i * step, step), step), :].astype(jnp.float32)
                for k, offset in places
            ]
            total = sum(jnp.sum(v * v, axis=1, keepdims=True) for v in values)
            scale = lax.rsqrt(total * (1.0 / (512 * NX)) + epsilon)
            for block, own_gain, v in zip(blocks, gains, values):
                columns = pl.ds(pl.multiple_of(block * 512, 512), 512)
                normed[there, columns] = (v * scale * own_gain).astype(jnp.bfloat16)
            return carry

        lax.fori_loop(0, count // step, normalise, 0, unroll=2 if count % (2 * step) == 0 else 1)
        base += count

    if n_pieces > 1:
        for piece, units in zip(pieces, units_of(c, 2 * c - 1)):
            for k, (mat, z_off, y_off) in enumerate(units):
                row = lax.rem(z + z_off + NZ, NZ) * 256 + lax.rem(y + y_off + NY, NY) * 64
                weights[mat, pl.ds(pl.multiple_of(row, 64), 64), :] = piece[k]
    else:
        for mat in range(3):
            whole(mat).wait()

    rows = normed.shape[0]
    same_before, same_after = same[:, 0:1] > 0.5, same[:, 1:2] > 0.5

    def mix(n, carry):
        columns = pl.ds(pl.multiple_of(n * 256, 256), 256)

        def project(mat):
            value = jnp.dot(normed[...], weights[mat, :, columns], preferred_element_type=jnp.float32)
            return value.astype(jnp.bfloat16).astype(jnp.float32)

        mixed = (project(0) * project(1)).astype(jnp.bfloat16).astype(jnp.float32)
        before = pltpu.roll(mixed, 1, 0)
        after = pltpu.roll(mixed, rows - 1, 0)
        convolved = (
            jnp.where(same_before, taps[0:1, columns] * before, 0.0)
            + taps[1:2, columns] * mixed
            + jnp.where(same_after, taps[2:3, columns] * after, 0.0)
        )
        gated[:, columns] = (project(2) * convolved).astype(jnp.bfloat16)
        return carry

    lax.fori_loop(0, 2, mix, 0)
    if n_pieces == 1:
        whole(3).wait()

    count = outs[0].shape[0]
    for off, out in ((2, outs[3]), (1, outs[1]), (-1, outs[2]), (0, outs[0])):
        block = lax.rem(x + off + NX, NX)

        def project_out(n, carry, block=block, out=out):
            rows = pl.ds(pl.multiple_of(block * 512 + n * 256, 256), 256)
            columns = pl.ds(pl.multiple_of(n * 256, 256), 256)
            out[:, columns] = lax.dot_general(
                gated[first : first + count, :],
                weights[3, rows, :],
                (((1,), (1,)), ((), ())),
                preferred_element_type=jnp.float32,
            ).astype(jnp.bfloat16)
            return carry

        lax.fori_loop(0, 2, project_out, 0)


def layer(sources, segments, kept, gain, same, taps, pieces):
    rows, count = sum(n for n, _ in segments), kept[1] - kept[0]
    vmem, hbm = pl.BlockSpec(memory_space=pltpu.VMEM), pl.BlockSpec(memory_space=pltpu.HBM)
    where = [hbm] if len(pieces) == 1 else [vmem] * len(pieces)
    return pl.pallas_call(
        functools.partial(layer_kernel, segments, len(sources), len(pieces), kept[0]),
        out_shape=[jax.ShapeDtypeStruct((count, 512), jnp.bfloat16)] * 4,
        in_specs=[vmem] * (len(sources) + 3) + where,
        out_specs=[vmem] * 4,
        scratch_shapes=[
            pltpu.VMEM((4, 2048, 512), jnp.bfloat16),
            pltpu.VMEM((rows, 2048), jnp.bfloat16),
            pltpu.VMEM((rows, 512), jnp.bfloat16),
            pltpu.SemaphoreType.DMA((4,)),
        ],
        compiler_params=pltpu.CompilerParams(vmem_limit_bytes=28 * 1024 * 1024),
        cost_estimate=pl.CostEstimate(flops=2 * rows * 2048 * 2048, bytes_accessed=8 << 20, transcendentals=rows),
    )(*sources, gain, same, taps, *pieces)


def per_device(stream, doc_ids, norm_gain, gate_proj, input_gate, value_proj, taps, out_proj):
    c = lax.axis_index("c")
    mats = jnp.stack([input_gate, value_proj, gate_proj, jnp.swapaxes(out_proj, 1, 2)], axis=1)
    second = lax.all_gather(mats[1], SP, axis=1, tiled=True)
    took = partner(mats[0])
    chip = jnp.concatenate([jnp.where(c == 0, mats[0], took), jnp.where(c == 0, took, mats[0])], axis=1)

    ids = jnp.broadcast_to(doc_ids.astype(jnp.bfloat16)[:, None], (doc_ids.shape[0], 128))
    wider = with_edges(jnp.concatenate([stream, ids], axis=1))
    rows = wider[:, :512]
    with jax.named_scope("ag_first"):
        left, right = shifted(rows, "x", 1), shifted(rows, "x", -1)
    me, length = lax.axis_index(SP), doc_ids.shape[0]
    docs = wider[:, 512].astype(jnp.float32)
    place = lax.broadcasted_iota(jnp.int32, (length + 2 * HALO,), 0) + me * length
    docs = jnp.where((place < HALO) | (place >= lax.axis_size(SP) * length + HALO), -1.0, docs)
    equal = (docs[1:] == docs[:-1]).astype(jnp.float32)
    none = jnp.zeros((1,), jnp.float32)
    same = jnp.stack([jnp.concatenate([none, equal]), jnp.concatenate([equal, none])], axis=1)
    gains = norm_gain.reshape(-1, NX, 512)
    first = gather_weights(chip, c)

    total = rows.shape[0]
    cut = (total // 32 + 1) * 16
    far_top, far_bottom = shifted(left[:cut], "x", 1), shifted(right[cut:], "x", -1)
    sources = (rows, left, right, far_top, far_bottom)
    top = lambda lo, hi: (hi - lo, ((0, lo), (1, lo), (2, lo), (3, lo)))
    bottom = lambda lo, hi: (hi - lo, ((0, lo), (1, lo), (2, lo), (4, lo - cut)))
    outs_a = layer(
        sources, (top(0, cut), bottom(cut, cut + 16)), (0, cut), gains[0], same[: cut + 16], taps[0], first
    )
    outs_b = layer(
        sources, (top(cut - 16, cut), bottom(cut, total)), (16, total - cut + 16),
        gains[0], same[cut - 16 :], taps[0], first,
    )
    chunk_a = scatter_x(rows[:cut], outs_a, 1)
    chunk_b = scatter_x(rows[cut:], outs_b, -1)

    got_a, got_b = gather_x(chunk_a, 1), gather_x(chunk_b, -1)
    of_a = lambda lo, hi: (hi - lo, tuple((k, lo) for k in range(4)))
    of_b = (total - cut, tuple((4 + k, 0) for k in range(4)))
    outs_a = layer(got_a, (of_a(0, cut),), (0, cut - 16), gains[1], same[:cut], taps[1], [second])
    outs_b = layer(
        got_a + got_b, (of_a(cut - 32, cut), of_b), (16, total - cut + 32),
        gains[1], same[cut - 32 :], taps[1], [second],
    )
    result_a = scatter_x(chunk_a[: cut - 16], outs_a, 1)
    result_b = scatter_x(jnp.concatenate([chunk_a[cut - 16 :], chunk_b], axis=0), outs_b, -1)
    return jnp.concatenate([result_a[HALO:], result_b[:-HALO]], axis=0)


def solution(mesh):
    split = Mesh(mesh.devices.reshape(NZ, NY, NC, NX), ("z", "y", "c", "x"))
    in_specs = (
        P(SP, "x"),
        P(SP),
        P(),
        P(None, SP, "x"),
        P(None, SP, "x"),
        P(None, SP, "x"),
        P(None, None, "x"),
        P(None, "x", SP),
    )
    return jax.shard_map(
        per_device, mesh=split, in_specs=in_specs, out_specs=P(SP, "x"), check_vma=False
    )
```

```python
import functools

import jax
import jax.numpy as jnp
from jax import lax
from jax.experimental import pallas as pl
from jax.experimental.pallas import tpu as pltpu
from jax.sharding import Mesh
from jax.sharding import PartitionSpec as P

epsilon = 1e-06
NZ, NY, NC, NX = 8, 4, 2, 4
SP = ("z", "y", "c")
HALO = 8


def partner(value):
    return lax.ppermute(value, "c", [(0, 1), (1, 0)])


def onward(value, axis, step=1):
    size = lax.axis_size(axis)
    pairs = [(2 * i, 2 * ((i + step) % size)) for i in range(size)]
    pairs += [(2 * i + 1, 2 * ((i - step) % size) + 1) for i in range(size)]
    return lax.ppermute(value, (axis, "c"), pairs)


def with_edges(value):
    size = lax.axis_size(SP)
    before = lax.ppermute(value[-HALO:], SP, [(i, i + 1) for i in range(size - 1)])
    after = lax.ppermute(value[:HALO], SP, [(i + 1, i) for i in range(size - 1)])
    return jnp.concatenate([before, value, after], axis=0)


def half(units, c):
    count = units.shape[0] // 2
    return lax.dynamic_slice_in_dim(units, c * count, count, axis=0)


def gather_weights(chip, c):
    around = lax.all_gather(chip[:2], "y", axis=0, tiled=True)
    moved = [around]
    for _ in range(3):
        moved.append(onward(moved[-1], "z"))
    moved = moved[1:] + [onward(half(moved[-1], c), "z")]
    pieces = [around] + moved + [partner(v) for v in moved]
    own = lax.all_gather(half(chip[2:], c), "z", axis=0, tiled=True)
    others = partner(own)
    near = onward(own, "y")
    moved = [near, onward(others, "y"), onward(near, "y")]
    return pieces + [own, others] + moved + [partner(v) for v in moved]


def units_of(y, z, c, s):
    both = [(m, y_at) for y_at in range(NY) for m in (0, 1)]

    def at_z(off):
        return lax.rem(z + off + NZ, NZ)

    def at_y(off):
        return lax.rem(y + off + NY, NY)

    def moved_a(c, s):
        full = [[(m, at_z(k * s), y_at) for m, y_at in both] for k in (1, 2, 3)]
        return full + [[(m, at_z(4), lax.rem(2 * c + k, NY)) for k in range(2) for m in (0, 1)]]

    def column(core, y_at):
        return [(2 + core, z_at, y_at) for z_at in range(NZ)]

    def moved_b(c, s):
        return [column(c, at_y(s)), column(1 - c, at_y(s)), column(c, at_y(2))]

    here_a = [[(m, z, y_at) for m, y_at in both]]
    here_b = [column(c, y), column(1 - c, y)]
    return here_a + moved_a(c, s) + moved_a(1 - c, -s) + here_b + moved_b(c, s) + moved_b(1 - c, -s)


def gather_x(rows):
    copies = jnp.broadcast_to(rows, (lax.axis_size("x"), *rows.shape))
    return lax.all_to_all(copies, "x", 0, 0, tiled=True)


def wide(value):
    return value.astype(jnp.float32)


def scatter_x(rows, parts):
    got = lax.all_to_all(parts, "x", 0, 0, tiled=True)
    return (wide(rows) + jnp.sum(wide(got), axis=0)).astype(jnp.bfloat16)


def layer_kernel(index, segments, kept, first, n_pieces, *refs):
    n_sources = 1 + max(k for _, (k, _) in segments)
    sources, refs = refs[:n_sources], refs[n_sources:]
    (gains, same_ref, taps), refs = refs[:3], refs[3:]
    pieces, refs = refs[:n_pieces], refs[n_pieces:]
    outs, (weights, normed, gated, sems) = refs[: len(kept)], refs[len(kept) :]
    y, z, c = (lax.axis_index(name) for name in ("y", "z", "c"))

    def whole(mat):
        return pltpu.make_async_copy(pieces[0].at[mat], weights.at[mat], sems.at[mat])

    if n_pieces == 1:
        for mat in range(4):
            whole(mat).start()

    step = 16
    base = 0
    for count, (k, offset) in segments:

        def normalise(i, carry, base=base, k=k, offset=offset):
            here = pl.ds(pl.multiple_of(offset + i * step, step), step)
            there = pl.ds(pl.multiple_of(base + i * step, step), step)
            values = [sources[k][block, here, :].astype(jnp.float32) for block in range(NX)]
            total = sum(jnp.sum(v * v, axis=1, keepdims=True) for v in values)
            scale = lax.rsqrt(total * (1.0 / (512 * NX)) + epsilon)
            for block, v in enumerate(values):
                scaled = v * scale * gains[index, block : block + 1, :]
                normed[there, block * 512 : (block + 1) * 512] = scaled.astype(jnp.bfloat16)
            return carry

        steps = count // step
        lax.fori_loop(0, steps, normalise, 0, unroll=next(u for u in (3, 2, 1) if steps % u == 0))
        base += count

    if n_pieces > 1:
        for piece, units in zip(pieces, units_of(y, z, c, 2 * c - 1)):
            for k, (mat, z_at, y_at) in enumerate(units):
                row = pl.multiple_of(z_at * 256 + y_at * 64, 64)
                weights[mat, pl.ds(row, 64), :] = piece[k]
    else:
        for mat in range(3):
            whole(mat).wait()

    rows = normed.shape[0]
    same = same_ref[first : first + rows, :]
    same_before, same_after = same[:, 0:1] > 0.5, same[:, 1:2] > 0.5

    def mix(n, carry):
        columns = pl.ds(pl.multiple_of(n * 256, 256), 256)

        def project(mat):
            value = jnp.dot(normed[...], weights[mat, :, columns], preferred_element_type=jnp.float32)
            return value.astype(jnp.bfloat16).astype(jnp.float32)

        mixed = (project(0) * project(1)).astype(jnp.bfloat16).astype(jnp.float32)
        before = pltpu.roll(mixed, 1, 0)
        after = pltpu.roll(mixed, rows - 1, 0)
        convolved = (
            jnp.where(same_before, taps[index, 0:1, columns] * before, 0.0)
            + taps[index, 1:2, columns] * mixed
            + jnp.where(same_after, taps[index, 2:3, columns] * after, 0.0)
        )
        gated[:, columns] = (project(2) * convolved).astype(jnp.bfloat16)
        return carry

    lax.fori_loop(0, 2, mix, 0)
    if n_pieces == 1:
        whole(3).wait()
    low, high = kept[0][0], kept[-1][1]

    def project_out(n, carry):
        value = lax.dot_general(
            gated[low:high, :],
            weights[3, pl.ds(pl.multiple_of(n * 256, 256), 256), :],
            (((1,), (1,)), ((), ())),
            preferred_element_type=jnp.float32,
        ).astype(jnp.bfloat16)
        columns = pl.ds(pl.multiple_of(lax.rem(n, 2) * 256, 256), 256)
        for out, (start, end) in zip(outs, kept):
            out[lax.div(n, 2), :, columns] = value[start - low : end - low]
        return carry

    lax.fori_loop(0, 2 * NX, project_out, 0)


def layer(index, sources, segments, kept, first, gains, same, taps, pieces):
    rows = sum(n for n, _ in segments)
    vmem = pl.BlockSpec(memory_space=pltpu.VMEM)
    where = [pl.BlockSpec(memory_space=pl.ANY)] if len(pieces) == 1 else [vmem] * len(pieces)
    return pl.pallas_call(
        functools.partial(layer_kernel, index, segments, kept, first, len(pieces)),
        out_shape=[jax.ShapeDtypeStruct((NX, end - start, 512), jnp.bfloat16) for start, end in kept],
        in_specs=[vmem] * (len(sources) + 3) + where,
        out_specs=[vmem] * len(kept),
        scratch_shapes=[
            pltpu.VMEM((4, 2048, 512), jnp.bfloat16),
            pltpu.VMEM((rows, 2048), jnp.bfloat16),
            pltpu.VMEM((rows, 512), jnp.bfloat16),
            pltpu.SemaphoreType.DMA((4,)),
        ],
        compiler_params=pltpu.CompilerParams(vmem_limit_bytes=(54 if len(pieces) == 1 else 32) << 20),
        cost_estimate=pl.CostEstimate(flops=2 * rows * 2048 * 2048, bytes_accessed=8 << 20, transcendentals=rows),
    )(*sources, gains, same, taps, *pieces)


def per_device(stream, doc_ids, norm_gain, gate_proj, input_gate, value_proj, taps, out_proj):
    c = lax.axis_index("c")
    mats = jnp.stack([input_gate, value_proj, gate_proj, jnp.swapaxes(out_proj, 1, 2)], axis=1)
    second = lax.all_gather(mats[1], SP, axis=1, tiled=True)
    chip = lax.all_gather(mats[0], "c", axis=1, tiled=True)

    ids = jnp.broadcast_to(doc_ids.astype(jnp.bfloat16)[:, None], (doc_ids.shape[0], 128))
    wider = with_edges(jnp.concatenate([stream, ids], axis=1))
    rows = wider[:, :512]
    gathered = gather_x(rows)
    me, length = lax.axis_index(SP), doc_ids.shape[0]
    docs = wider[:, 512].astype(jnp.float32)
    place = lax.broadcasted_iota(jnp.int32, (length + 2 * HALO,), 0) + me * length
    docs = jnp.where((place < HALO) | (place >= lax.axis_size(SP) * length + HALO), -1.0, docs)
    equal = (docs[1:] == docs[:-1]).astype(jnp.float32)
    none = jnp.zeros((1,), jnp.float32)
    same = jnp.stack([jnp.concatenate([none, equal]), jnp.concatenate([equal, none])], axis=1)
    gains = norm_gain.reshape(-1, NX, 512)
    first = gather_weights(chip, c)

    total = rows.shape[0]
    cut = (total // 32 + 1) * 16
    kept = ((0, cut), (cut, total))
    parts_a, parts_b = layer(0, [gathered], ((total, (0, 0)),), kept, 0, gains, same, taps, first)
    chunk_a, chunk_b = scatter_x(rows[:cut], parts_a), scatter_x(rows[cut:], parts_b)

    got = [gather_x(chunk_a), gather_x(chunk_b)]
    kept = ((0, cut - 16),)
    (parts_a,) = layer(1, got[:1], ((cut, (0, 0)),), kept, 0, gains, same, taps, [second])
    segments, kept = ((32, (0, cut - 32)), (total - cut, (1, 0))), ((16, total - cut + 32),)
    (parts_b,) = layer(1, got, segments, kept, cut - 32, gains, same, taps, [second])
    result_a = scatter_x(chunk_a[: cut - 16], parts_a)
    result_b = scatter_x(jnp.concatenate([chunk_a[cut - 16 :], chunk_b], axis=0), parts_b)
    return jnp.concatenate([result_a[HALO:], result_b[:-HALO]], axis=0)


def solution(mesh):
    split = Mesh(mesh.devices.reshape(NZ, NY, NC, NX), ("z", "y", "c", "x"))
    in_specs = (
        P(SP, "x"),
        P(SP),
        P(),
        P(None, SP, "x"),
        P(None, SP, "x"),
        P(None, SP, "x"),
        P(None, None, "x"),
        P(None, "x", SP),
    )
    return jax.shard_map(
        per_device, mesh=split, in_specs=in_specs, out_specs=P(SP, "x"), check_vma=False
    )
```

```python
import functools

import jax
import jax.numpy as jnp
from jax import lax
from jax.experimental import pallas as pl
from jax.experimental.pallas import tpu as pltpu
from jax.sharding import Mesh
from jax.sharding import PartitionSpec as P

epsilon = 1e-06
NZ, NY, NC, NX = 8, 4, 2, 4
SP = ("z", "y", "c")
HALO = 8
VMEM_FIRST, VMEM_LATE = 24, 14


def partner(value):
    return lax.ppermute(value, "c", [(0, 1), (1, 0)])


def onward(value, axis, step=1):
    size = lax.axis_size(axis)
    pairs = [(2 * i, 2 * ((i + step) % size)) for i in range(size)]
    pairs += [(2 * i + 1, 2 * ((i - step) % size) + 1) for i in range(size)]
    return lax.ppermute(value, (axis, "c"), pairs)


def shifted(value, axis, step):
    size = lax.axis_size(axis)
    return lax.ppermute(value, axis, [(i, (i + step) % size) for i in range(size)])


def with_edges(value, c):
    size = lax.axis_size(SP)
    first, last = value[:HALO], value[-HALO:]
    both = lax.all_gather(jnp.concatenate([first, last], axis=0), "c", axis=0)
    pairs = [(i, i - 1) for i in range(2, size, 2)] + [(i, i + 1) for i in range(1, size - 1, 2)]
    outer = lax.ppermute(jnp.where(c == 0, first, last), SP, pairs)
    before = jnp.where(c == 0, outer, both[0, HALO:])
    after = jnp.where(c == 0, both[1, :HALO], outer)
    return jnp.concatenate([before, value, after], axis=0)


def half(units, c):
    count = units.shape[0] // 2
    return lax.dynamic_slice_in_dim(units, c * count, count, axis=0)


def gather_weights(chip, c):
    own = chip[:2]
    mixed = jnp.concatenate([half(own, c), onward(own, "y"), onward(half(own, c), "y", 2)], axis=0)
    around = lax.all_gather(mixed, "c", axis=0, tiled=True)
    moved = [around]
    for _ in range(3):
        moved.append(onward(moved[-1], "z"))
    moved = moved[1:] + [onward(half(moved[-1], c), "z")]
    pieces = [around] + moved + [partner(jnp.concatenate(moved[k : k + 2], axis=0)) for k in (0, 2)]
    own = chip[2:]
    one, two = onward(own, "z"), onward(own, "z", 2)
    far = onward(jnp.concatenate([one, half(two, c)], axis=0), "z", 2)
    side = jnp.concatenate([half(own, c), one, two, far], axis=0)
    around = jnp.concatenate([partner(side), side], axis=0)
    near = onward(around, "y")
    moved = [near, onward(near[near.shape[0] // 2 :], "y")]
    return pieces + [around] + moved + [partner(jnp.concatenate(moved, axis=0))]


def units_of(y, z, c, s):
    def mixed(c, s):
        return [(c, 0), (0, s), (1, s), (c, 2)]

    def side(c, s):
        return [(2 + c, 0)] + [(m, k * s) for k in (1, 2, 3) for m in (2, 3)] + [(2 + c, 4)]

    both = mixed(0, -1) + mixed(1, 1)

    def a(units, off):
        return [(m, lax.rem(z + off + NZ, NZ), lax.rem(y + y_off + NY, NY)) for m, y_off in units]

    def b(units, off):
        return [(m, lax.rem(z + z_off + NZ, NZ), lax.rem(y + off + NY, NY)) for m, z_off in units]

    def moved_a(c, s):
        return [a(both, k * s) for k in (1, 2, 3)] + [a(mixed(c, s), 4)]

    def around_b(c, s):
        return side(1 - c, -s) + side(c, s)

    def moved_b(c, s):
        return [b(around_b(c, s), s), b(side(c, s), 2)]

    theirs_a, theirs_b = moved_a(1 - c, -s), moved_b(1 - c, -s)
    first = [a(both, 0)] + moved_a(c, s) + [theirs_a[0] + theirs_a[1], theirs_a[2] + theirs_a[3]]
    return first + [b(around_b(c, s), 0)] + moved_b(c, s) + [theirs_b[0] + theirs_b[1]]


def gather_first(rows):
    copies = jnp.broadcast_to(rows, (lax.axis_size("x"), *rows.shape))
    return lax.all_to_all(copies, "x", 0, 0, tiled=True)


def gather_x(rows, way):
    left, right = shifted(rows, "x", 1), shifted(rows, "x", -1)
    return [rows, left, right, shifted(left if way == 1 else right, "x", way)]


def wide(value):
    return value.astype(jnp.float32)


def joined(near, far):
    return (wide(near) + wide(far)).astype(jnp.bfloat16)


def scatter_first(rows, own, right, left, far_top, far_bottom):
    cut = far_top.shape[0]
    right_top = joined(right[:cut], shifted(far_top, "x", 1))
    left_bottom = joined(left[cut:], shifted(far_bottom, "x", -1))
    from_left = shifted(jnp.concatenate([right_top, right[cut:]], axis=0), "x", 1)
    from_right = shifted(jnp.concatenate([left[:cut], left_bottom], axis=0), "x", -1)

    def total(part):
        got = wide(own[part]) + wide(from_left[part]) + wide(from_right[part])
        return (wide(rows[part]) + got).astype(jnp.bfloat16)

    return total(slice(None, cut)), total(slice(cut, None))


def scatter_x(rows, parts, way):
    own, right, left, far = parts
    got = shifted(far, "x", way)
    right, left = (joined(right, got), left) if way == 1 else (right, joined(left, got))
    from_left, from_right = shifted(right, "x", 1), shifted(left, "x", -1)
    return (wide(rows) + (wide(own) + wide(from_left) + wide(from_right))).astype(jnp.bfloat16)


def layer_kernel(index, segments, kept, first, n_sources, n_pieces, *refs):
    sources, refs = refs[:n_sources], refs[n_sources:]
    (gains, same_ref, taps), refs = refs[:3], refs[3:]
    pieces, refs = refs[:n_pieces], refs[n_pieces:]
    outs, refs = refs[: 3 + len(kept)], refs[3 + len(kept) :]
    (normed, gated), weights = refs[:2], (refs[2] if n_pieces > 1 else pieces[0])
    x, y, z, c = (lax.axis_index(name) for name in ("x", "y", "z", "c"))
    blocks = [lax.rem(x + off + NX, NX) for off in (0, -1, 1, 2)] if n_sources > 1 else list(range(NX))

    step = 16
    base = 0
    for count, k, offset in segments:

        def normalise(i, carry, base=base, k=k, offset=offset):
            here = pl.ds(pl.multiple_of(offset + i * step, step), step)
            there = pl.ds(pl.multiple_of(base + i * step, step), step)
            if n_sources > 1:
                values = [source[here, :].astype(jnp.float32) for source in sources[4 * k : 4 * k + 4]]
            else:
                values = [sources[0][block, here, :].astype(jnp.float32) for block in blocks]
            total = sum(jnp.sum(v * v, axis=1, keepdims=True) for v in values)
            scale = lax.rsqrt(total * (1.0 / (512 * NX)) + epsilon)
            for block, v in zip(blocks, values):
                columns = pl.ds(pl.multiple_of(block * 512, 512), 512)
                scaled = v * scale * gains[index, pl.ds(block, 1), :]
                normed[there, columns] = scaled.astype(jnp.bfloat16)
            return carry

        steps = count // step
        lax.fori_loop(0, steps, normalise, 0, unroll=next(u for u in (3, 2, 1) if steps % u == 0))
        base += count

    if n_pieces > 1:
        for piece, units in zip(pieces, units_of(y, z, c, 2 * c - 1)):
            for k, (mat, z_at, y_at) in enumerate(units):
                row = pl.multiple_of(z_at * 256 + y_at * 64, 64)
                weights[mat, pl.ds(row, 64), :] = piece[k]

    rows = normed.shape[0]
    same = same_ref[first : first + rows, :]
    same_before, same_after = same[:, 0:1] > 0.5, same[:, 1:2] > 0.5

    def mix(n, carry):
        columns = pl.ds(pl.multiple_of(n * 256, 256), 256)

        def project(mat):
            value = jnp.dot(normed[...], weights[mat, :, columns], preferred_element_type=jnp.float32)
            return value.astype(jnp.bfloat16).astype(jnp.float32)

        mixed = (project(0) * project(1)).astype(jnp.bfloat16).astype(jnp.float32)
        before = pltpu.roll(mixed, 1, 0)
        after = pltpu.roll(mixed, rows - 1, 0)
        convolved = (
            jnp.where(same_before, taps[index, 0:1, columns] * before, 0.0)
            + taps[index, 1:2, columns] * mixed
            + jnp.where(same_after, taps[index, 2:3, columns] * after, 0.0)
        )
        gated[:, columns] = (project(2) * convolved).astype(jnp.bfloat16)
        return carry

    lax.fori_loop(0, 2, mix, 0)
    low, high = kept[0][0], kept[-1][1]

    for place, off in enumerate((0, 1, -1, 2)):
        block = lax.rem(x + off + NX, NX)

        def project_out(n, carry, place=place, block=block):
            value = lax.dot_general(
                gated[low:high, :],
                weights[3, pl.ds(pl.multiple_of(block * 512 + n * 256, 256), 256), :],
                (((1,), (1,)), ((), ())),
                preferred_element_type=jnp.float32,
            ).astype(jnp.bfloat16)
            columns = pl.ds(pl.multiple_of(n * 256, 256), 256)
            if place < 3:
                outs[place][:, columns] = value
            else:
                for out, (start, end) in zip(outs[3:], kept):
                    out[:, columns] = value[start - low : end - low]
            return carry

        lax.fori_loop(0, 2, project_out, 0)


def layer(index, sources, segments, kept, first, gains, same, taps, pieces):
    rows = sum(n for n, _, _ in segments)
    vmem = pl.BlockSpec(memory_space=pltpu.VMEM)
    scratch = [pltpu.VMEM((rows, 2048), jnp.bfloat16), pltpu.VMEM((rows, 512), jnp.bfloat16)]
    if len(pieces) > 1:
        scratch.append(pltpu.VMEM((4, 2048, 512), jnp.bfloat16))
    counts = (kept[-1][1] - kept[0][0],) * 3 + tuple(end - start for start, end in kept)
    return pl.pallas_call(
        functools.partial(layer_kernel, index, segments, kept, first, len(sources), len(pieces)),
        out_shape=[jax.ShapeDtypeStruct((n, 512), jnp.bfloat16) for n in counts],
        in_specs=[vmem] * (len(sources) + 3 + len(pieces)),
        out_specs=[vmem] * len(counts),
        scratch_shapes=scratch,
        compiler_params=pltpu.CompilerParams(vmem_limit_bytes=(VMEM_LATE if len(pieces) == 1 else VMEM_FIRST) << 20),
        cost_estimate=pl.CostEstimate(flops=2 * rows * 2048 * 2048, bytes_accessed=8 << 20, transcendentals=rows),
    )(*sources, gains, same, taps, *pieces)


def per_device(stream, doc_ids, norm_gain, gate_proj, input_gate, value_proj, taps, out_proj):
    c = lax.axis_index("c")
    mats = jnp.stack([input_gate, value_proj, gate_proj, jnp.swapaxes(out_proj, 1, 2)], axis=1)
    second = lax.all_gather(mats[1], SP, axis=1, tiled=True)
    chip = lax.all_gather(mats[0], "c", axis=1, tiled=True)

    ids = jnp.broadcast_to(doc_ids.astype(jnp.bfloat16)[:, None], (doc_ids.shape[0], 128))
    wider = with_edges(jnp.concatenate([stream, ids], axis=1), c)
    rows = wider[:, :512]
    gathered = gather_first(rows)
    me, length = lax.axis_index(SP), doc_ids.shape[0]
    docs = wider[:, 512].astype(jnp.float32)
    place = lax.broadcasted_iota(jnp.int32, (length + 2 * HALO,), 0) + me * length
    docs = jnp.where((place < HALO) | (place >= lax.axis_size(SP) * length + HALO), -1.0, docs)
    equal = (docs[1:] == docs[:-1]).astype(jnp.float32)
    none = jnp.zeros((1,), jnp.float32)
    same = jnp.stack([jnp.concatenate([none, equal]), jnp.concatenate([equal, none])], axis=1)
    gains = norm_gain.reshape(-1, NX, 512)
    first = gather_weights(chip, c)

    total = rows.shape[0]
    cut = (total // 32 + 1) * 16
    kept = ((0, cut), (cut, total))
    parts = layer(0, [gathered], ((total, 0, 0),), kept, 0, gains, same, taps, first)
    chunk_a, chunk_b = scatter_first(rows, *parts)

    got_a, got_b = gather_x(chunk_a, 1), gather_x(chunk_b, -1)
    parts_a = layer(1, got_a, ((cut, 0, 0),), ((0, cut - 16),), 0, gains, same, taps, [second])
    segments, kept = ((32, 0, cut - 32), (total - cut, 1, 0)), ((16, total - cut + 32),)
    parts_b = layer(1, got_a + got_b, segments, kept, cut - 32, gains, same, taps, [second])
    result_a = scatter_x(chunk_a[: cut - 16], parts_a, 1)
    result_b = scatter_x(jnp.concatenate([chunk_a[cut - 16 :], chunk_b], axis=0), parts_b, -1)
    return jnp.concatenate([result_a[HALO:], result_b[:-HALO]], axis=0)


def solution(mesh):
    split = Mesh(mesh.devices.reshape(NZ, NY, NC, NX), ("z", "y", "c", "x"))
    in_specs = (
        P(SP, "x"),
        P(SP),
        P(),
        P(None, SP, "x"),
        P(None, SP, "x"),
        P(None, SP, "x"),
        P(None, None, "x"),
        P(None, "x", SP),
    )
    return jax.shard_map(
        per_device, mesh=split, in_specs=in_specs, out_specs=P(SP, "x"), check_vma=False
    )
```

```python
import functools

import jax
import jax.numpy as jnp
from jax import lax
from jax.experimental import pallas as pl
from jax.experimental.pallas import tpu as pltpu
from jax.sharding import Mesh
from jax.sharding import PartitionSpec as P


epsilon = 1e-06
NZ, NY, NC, NX = 8, 4, 2, 4
SP = ("z", "y", "c")
HALO = 8
VMEM_LIMIT = 26


def partner(value):
    return lax.ppermute(value, "c", [(0, 1), (1, 0)])


def onward(value, axis, step=1):
    size = lax.axis_size(axis)
    pairs = [(2 * i, 2 * ((i + step) % size)) for i in range(size)]
    pairs += [(2 * i + 1, 2 * ((i - step) % size) + 1) for i in range(size)]
    return lax.ppermute(value, (axis, "c"), pairs)


def shifted(value, axis, step):
    size = lax.axis_size(axis)
    return lax.ppermute(value, axis, [(i, (i + step) % size) for i in range(size)])


def with_edges(value, c):
    size = lax.axis_size(SP)
    first, last = value[:HALO], value[-HALO:]
    both = lax.all_gather(jnp.concatenate([first, last], axis=0), "c", axis=0)
    pairs = [(i, i - 1) for i in range(2, size, 2)] + [(i, i + 1) for i in range(1, size - 1, 2)]
    outer = lax.ppermute(jnp.where(c == 0, first, last), SP, pairs)
    before = jnp.where(c == 0, outer, both[0, HALO:])
    after = jnp.where(c == 0, both[1, :HALO], outer)
    return jnp.concatenate([before, value, after], axis=0)


def half(units, c):
    count = units.shape[0] // 2
    return lax.dynamic_slice_in_dim(units, c * count, count, axis=0)


def by_y_then_z(own, c):
    near = onward(own, "y")
    opposite = onward(half(own, c), "y", 2)
    mixed = jnp.concatenate([half(own, c), near, opposite], axis=0)
    if own.shape[0] == 2:
        around = lax.all_gather(mixed, "c", axis=0, tiled=True)
    else:
        other = partner(mixed)
        around = jnp.where(c == 0, jnp.concatenate([mixed, other]), jnp.concatenate([other, mixed]))
    moved = [around]
    for _ in range(3):
        moved.append(onward(moved[-1], "z"))
    moved = moved[1:] + [onward(half(moved[-1], c), "z")]
    return [around] + moved + [partner(jnp.concatenate(moved[k : k + 2], axis=0)) for k in (0, 2)]


def by_z_then_y(own, c):
    one = onward(own, "z")
    two = onward(own, "z", 2)
    far = onward(jnp.concatenate([one, half(two, c)], axis=0), "z", 2)
    side = jnp.concatenate([half(own, c), one, two, far], axis=0)
    side = lax.optimization_barrier(side)
    around = jnp.concatenate([partner(side), side], axis=0)
    near = onward(around, "y")
    moved = [near, onward(near[near.shape[0] // 2 :], "y")]
    return [around] + moved + [partner(jnp.concatenate(moved, axis=0))]


def units_of(layer_index, y, z, c, s):
    def a(units, off):
        return [(m, lax.rem(z + off + NZ, NZ), lax.rem(y + y_off + NY, NY)) for m, y_off in units]

    def b(units, off):
        return [(m, lax.rem(z + z_off + NZ, NZ), lax.rem(y + off + NY, NY)) for m, z_off in units]

    count = 1 if layer_index == 0 else 2

    def mixed(c, s):
        halves = [count * c + k for k in range(count)]
        near = [(m, s) for m in range(2 * count)]
        return [(m, 0) for m in halves] + near + [(m, 2) for m in halves]

    both = mixed(0, -1) + mixed(1, 1)

    def moved_a(c, s):
        return [a(both, k * s) for k in (1, 2, 3)] + [a(mixed(c, s), 4)]

    theirs = moved_a(1 - c, -s)
    first = [a(both, 0)] + moved_a(c, s) + [theirs[0] + theirs[1], theirs[2] + theirs[3]]
    if layer_index == 1:
        return first

    def side(c, s):
        return [(2 + c, 0)] + [(m, k * s) for k in (1, 2, 3) for m in (2, 3)] + [(2 + c, 4)]

    def around_b(c, s):
        return side(1 - c, -s) + side(c, s)

    def moved_b(c, s):
        return [b(around_b(c, s), s), b(side(c, s), 2)]

    theirs = moved_b(1 - c, -s)
    return first + [b(around_b(c, s), 0)] + moved_b(c, s) + [theirs[0] + theirs[1]]


def gather_first(rows):
    copies = jnp.broadcast_to(rows, (lax.axis_size("x"), *rows.shape))
    return lax.all_to_all(copies, "x", 0, 0, tiled=True)


def gather_x(rows, cut):
    left = shifted(rows, "x", 1)
    right = shifted(rows, "x", -1)
    return [rows, left, right, shifted(left[:cut], "x", 1), shifted(right[cut:], "x", -1)]


def wide(value):
    return value.astype(jnp.float32)


def joined(near, far):
    return (wide(near) + wide(far)).astype(jnp.bfloat16)


def scatter_x(rows, own, right, left, far_top, far_bottom):
    cut = far_top.shape[0]
    got_top = shifted(far_top, "x", 1)
    got_bottom = shifted(far_bottom, "x", -1)
    right = jnp.concatenate([joined(right[:cut], got_top), right[cut:]], axis=0)
    left = jnp.concatenate([left[:cut], joined(left[cut:], got_bottom)], axis=0)
    from_left = shifted(right, "x", 1)
    from_right = shifted(left, "x", -1)
    return (wide(rows) + (wide(own) + wide(from_left) + wide(from_right))).astype(jnp.bfloat16)


def layer_kernel(index, cut, n_sources, n_pieces, *refs):
    sources, refs = refs[:n_sources], refs[n_sources:]
    (gains, same_ref, taps), refs = refs[:3], refs[3:]
    pieces, refs = refs[:n_pieces], refs[n_pieces:]
    outs, (normed, gated, weights) = refs[:5], refs[5:]
    x, y, z, c = (lax.axis_index(name) for name in ("x", "y", "z", "c"))
    blocks = [lax.rem(x + off + NX, NX) for off in (0, -1, 1, 2)] if n_sources > 1 else list(range(NX))

    step = 16
    for base, count in ((0, cut), (cut, normed.shape[0] - cut)):

        def normalise(i, carry, base=base):
            here = pl.ds(pl.multiple_of(i * step, step), step)
            there = pl.ds(pl.multiple_of(base + i * step, step), step)
            if n_sources > 1:
                values = [source[there, :].astype(jnp.float32) for source in sources[:3]]
                values.append(sources[3 if base == 0 else 4][here, :].astype(jnp.float32))
            else:
                values = [sources[0][block, there, :].astype(jnp.float32) for block in blocks]
            total = sum(jnp.sum(v * v, axis=1, keepdims=True) for v in values)
            scale = lax.rsqrt(total * (1.0 / (512 * NX)) + epsilon)
            for block, v in zip(blocks, values):
                columns = pl.ds(pl.multiple_of(block * 512, 512), 512)
                scaled = v * scale * gains[index, pl.ds(block, 1), :]
                normed[there, columns] = scaled.astype(jnp.bfloat16)
            return carry

        steps = count // step
        lax.fori_loop(0, steps, normalise, 0, unroll=2 if steps % 2 == 0 else 1)

    for piece, units in zip(pieces, units_of(index, y, z, c, 2 * c - 1)):
        for k, (mat, z_at, y_at) in enumerate(units):
            row = pl.multiple_of(z_at * 256 + y_at * 64, 64)
            weights[mat, pl.ds(row, 64), :] = piece[k]

    rows = normed.shape[0]
    same = same_ref[...]
    same_before, same_after = same[:, 0:1] > 0.5, same[:, 1:2] > 0.5

    def mix(n, carry):
        columns = pl.ds(pl.multiple_of(n * 256, 256), 256)

        def project(mat):
            value = jnp.dot(normed[...], weights[mat, :, columns], preferred_element_type=jnp.float32)
            return value.astype(jnp.bfloat16).astype(jnp.float32)

        mixed = (project(0) * project(1)).astype(jnp.bfloat16).astype(jnp.float32)
        before = pltpu.roll(mixed, 1, 0)
        after = pltpu.roll(mixed, rows - 1, 0)
        convolved = (
            jnp.where(same_before, taps[index, 0:1, columns] * before, 0.0)
            + taps[index, 1:2, columns] * mixed
            + jnp.where(same_after, taps[index, 2:3, columns] * after, 0.0)
        )
        gated[:, columns] = (project(2) * convolved).astype(jnp.bfloat16)
        return carry

    lax.fori_loop(0, 2, mix, 0)

    for place, off in enumerate((0, 1, -1, 2)):
        block = lax.rem(x + off + NX, NX)

        def project_out(n, carry, place=place, block=block):
            value = lax.dot_general(
                gated[...],
                weights[3, pl.ds(pl.multiple_of(block * 512 + n * 256, 256), 256), :],
                (((1,), (1,)), ((), ())),
                preferred_element_type=jnp.float32,
            ).astype(jnp.bfloat16)
            columns = pl.ds(pl.multiple_of(n * 256, 256), 256)
            if place < 3:
                outs[place][:, columns] = value
            else:
                outs[3][:, columns] = value[:cut]
                outs[4][:, columns] = value[cut:]
            return carry

        lax.fori_loop(0, 2, project_out, 0)


def layer(index, cut, sources, gains, same, taps, pieces):
    rows = same.shape[0]
    vmem = pl.BlockSpec(memory_space=pltpu.VMEM)
    return pl.pallas_call(
        functools.partial(layer_kernel, index, cut, len(sources), len(pieces)),
        out_shape=[jax.ShapeDtypeStruct((n, 512), jnp.bfloat16) for n in (rows, rows, rows, cut, rows - cut)],
        in_specs=[vmem] * (len(sources) + 3 + len(pieces)),
        out_specs=[vmem] * 5,
        scratch_shapes=[
            pltpu.VMEM((rows, 2048), jnp.bfloat16),
            pltpu.VMEM((rows, 512), jnp.bfloat16),
            pltpu.VMEM((4, 2048, 512), jnp.bfloat16),
        ],
        compiler_params=pltpu.CompilerParams(vmem_limit_bytes=VMEM_LIMIT << 20),
        cost_estimate=pl.CostEstimate(flops=2 * rows * 2048 * 2048, bytes_accessed=8 << 20, transcendentals=rows),
    )(*sources, gains, same, taps, *pieces)


def per_device(stream, doc_ids, norm_gain, gate_proj, input_gate, value_proj, taps, out_proj):
    c = lax.axis_index("c")
    mats = jnp.stack([input_gate, value_proj, gate_proj, jnp.swapaxes(out_proj, 1, 2)], axis=1)
    chip = lax.all_gather(mats, "c", axis=2, tiled=True)

    ids = jnp.broadcast_to(doc_ids.astype(jnp.bfloat16)[:, None], (doc_ids.shape[0], 128))
    wider = with_edges(jnp.concatenate([stream, ids], axis=1), c)
    rows = wider[:, :512]
    gathered = gather_first(rows)
    me, length = lax.axis_index(SP), doc_ids.shape[0]
    docs = wider[:, 512].astype(jnp.float32)
    place = lax.broadcasted_iota(jnp.int32, (length + 2 * HALO,), 0) + me * length
    docs = jnp.where((place < HALO) | (place >= lax.axis_size(SP) * length + HALO), -1.0, docs)
    equal = (docs[1:] == docs[:-1]).astype(jnp.float32)
    none = jnp.zeros((1,), jnp.float32)
    same = jnp.stack([jnp.concatenate([none, equal]), jnp.concatenate([equal, none])], axis=1)
    gains = norm_gain.reshape(-1, NX, 512)
    pieces = [by_y_then_z(chip[0, :2], c) + by_z_then_y(chip[0, 2:], c), by_y_then_z(chip[1], c)]

    cut = (rows.shape[0] // 32 + 1) * 16
    sources = [gathered]
    for index in range(2):
        parts = layer(index, cut, sources, gains, same, taps, pieces[index])
        rows = scatter_x(rows, *parts)
        if index == 0:
            sources = gather_x(rows, cut)
    return rows[HALO:-HALO]


def solution(mesh):
    split = Mesh(mesh.devices.reshape(NZ, NY, NC, NX), ("z", "y", "c", "x"))
    in_specs = (
        P(SP, "x"),
        P(SP),
        P(),
        P(None, SP, "x"),
        P(None, SP, "x"),
        P(None, SP, "x"),
        P(None, None, "x"),
        P(None, "x", SP),
    )

    return jax.shard_map(per_device, mesh=split, in_specs=in_specs, out_specs=P(SP, "x"), check_vma=False)
```

```python
import functools

import jax
import jax.numpy as jnp
from jax import lax
from jax.experimental import pallas as pl
from jax.experimental.pallas import tpu as pltpu
from jax.sharding import Mesh
from jax.sharding import PartitionSpec as P


epsilon = 1e-06
NZ, NY, NC, NX = 8, 4, 2, 4
SP = ("z", "y", "c")
HALO = 8
VMEM_LIMIT = 22


def partner(value):
    return lax.ppermute(value, "c", [(0, 1), (1, 0)])


def onward(value, axis, step=1):
    size = lax.axis_size(axis)
    pairs = [(2 * i, 2 * ((i + step) % size)) for i in range(size)]
    pairs += [(2 * i + 1, 2 * ((i - step) % size) + 1) for i in range(size)]
    return lax.ppermute(value, (axis, "c"), pairs)


def shifted(value, axis, step):
    size = lax.axis_size(axis)
    return lax.ppermute(value, axis, [(i, (i + step) % size) for i in range(size)])


def with_edges(value, c):
    size = lax.axis_size(SP)
    first, last = value[:HALO], value[-HALO:]
    both = lax.all_gather(jnp.concatenate([first, last], axis=0), "c", axis=0)
    pairs = [(i, i - 1) for i in range(2, size, 2)] + [(i, i + 1) for i in range(1, size - 1, 2)]
    outer = lax.ppermute(jnp.where(c == 0, first, last), SP, pairs)
    before = jnp.where(c == 0, outer, both[0, HALO:])
    after = jnp.where(c == 0, both[1, :HALO], outer)
    return jnp.concatenate([before, value, after], axis=0)


def half(units, c):
    count = units.shape[0] // 2
    return lax.dynamic_slice_in_dim(units, c * count, count, axis=0)


def by_y_then_z(own, c):
    near = onward(own, "y")
    opposite = onward(half(own, c), "y", 2)
    mixed = jnp.concatenate([half(own, c), near, opposite], axis=0)
    if own.shape[0] == 2:
        around = lax.all_gather(mixed, "c", axis=0, tiled=True)
    else:
        mixed = lax.optimization_barrier(mixed)
        other = partner(mixed)
        around = jnp.concatenate([other, mixed], axis=0)
    moved = [around]
    for _ in range(3):
        moved.append(onward(moved[-1], "z"))
    last = half(moved[-1], c) if own.shape[0] == 2 else moved[-1][mixed.shape[0] :]
    moved = moved[1:] + [onward(last, "z")]
    if own.shape[0] == 2:
        swapped = [partner(jnp.concatenate(moved[:2], axis=0))]
        swapped += [partner(moved[2]), partner(moved[3])]
    else:
        swapped = []
        for k in (0, 2):
            swapped.append(partner(jnp.concatenate(moved[k : k + 2], axis=0)))
    return [around] + moved + swapped


def by_z_then_y(own, c):
    one = onward(own, "z")
    two = onward(own, "z", 2)
    far = onward(jnp.concatenate([one, half(two, c)], axis=0), "z", 2)
    side = jnp.concatenate([half(own, c), one, two, far], axis=0)
    side = lax.optimization_barrier(side)
    other = partner(side)
    around = jnp.concatenate([other, side], axis=0)
    near = onward(around, "y")
    moved = [near, onward(near[near.shape[0] // 2 :], "y")]
    swapped = partner(jnp.concatenate(moved, axis=0))
    return [around] + moved + [swapped]


def units_of(layer_index, y, z, c, s):
    def a(units, off):
        return [(m, lax.rem(z + off + NZ, NZ), lax.rem(y + y_off + NY, NY)) for m, y_off in units]

    def b(units, off):
        return [(m, lax.rem(z + z_off + NZ, NZ), lax.rem(y + off + NY, NY)) for m, z_off in units]

    count = 1 if layer_index == 0 else 2

    def mixed(c, s):
        halves = [count * c + k for k in range(count)]
        near = [(m, s) for m in range(2 * count)]
        return [(m, 0) for m in halves] + near + [(m, 2) for m in halves]

    def both(c, s):
        return mixed(0, -1) + mixed(1, 1) if layer_index == 0 else mixed(1 - c, -s) + mixed(c, s)

    def moved_a(c, s):
        return [a(both(c, s), k * s) for k in (1, 2, 3)] + [a(mixed(c, s), 4)]

    theirs = moved_a(1 - c, -s)
    first = [a(both(c, s), 0)] + moved_a(c, s) + [theirs[0] + theirs[1]]
    if layer_index == 1:
        return first + [theirs[2] + theirs[3]]
    first += theirs[2:]

    def side(c, s):
        return [(2 + c, 0)] + [(m, k * s) for k in (1, 2, 3) for m in (2, 3)] + [(2 + c, 4)]

    def around_b(c, s):
        return side(1 - c, -s) + side(c, s)

    def moved_b(c, s):
        return [b(around_b(c, s), s), b(side(c, s), 2)]

    theirs = moved_b(1 - c, -s)
    return first + [b(around_b(c, s), 0)] + moved_b(c, s) + [theirs[0] + theirs[1]]


def gather_first(rows):
    copies = jnp.broadcast_to(rows, (lax.axis_size("x"), *rows.shape))
    return lax.all_to_all(copies, "x", 0, 0, tiled=True)


def gather_x(rows, cut):
    left = shifted(rows, "x", 1)
    right = shifted(rows, "x", -1)
    far_top = shifted(left[:cut], "x", 1)
    far_bottom = shifted(right[cut:], "x", -1)
    return [rows, left, right, far_top, far_bottom]


def wide(value):
    return value.astype(jnp.float32)


def joined(near, far):
    return (wide(near) + wide(far)).astype(jnp.bfloat16)


def scatter_x(rows, own, right, left, far_top, far_bottom):
    cut = far_top.shape[0]
    got_top = shifted(far_top, "x", 1)
    got_bottom = shifted(far_bottom, "x", -1)
    right = jnp.concatenate([joined(right[:cut], got_top), right[cut:]], axis=0)
    left = jnp.concatenate([left[:cut], joined(left[cut:], got_bottom)], axis=0)
    from_left = shifted(right, "x", 1)
    from_right = shifted(left, "x", -1)
    return (wide(rows) + (wide(own) + wide(from_left) + wide(from_right))).astype(jnp.bfloat16)


def layer_kernel(index, cut, n_sources, n_pieces, *refs):
    sources, refs = refs[:n_sources], refs[n_sources:]
    (gains, same_ref, taps), refs = refs[:3], refs[3:]
    pieces, refs = refs[:n_pieces], refs[n_pieces:]
    outs, (normed, gated, weights) = refs[:5], refs[5:]
    x, y, z, c = (lax.axis_index(name) for name in ("x", "y", "z", "c"))
    blocks = [lax.rem(x + off + NX, NX) for off in (0, -1, 1, 2)] if n_sources > 1 else list(range(NX))

    step = 16
    for base, count in ((0, cut), (cut, normed.shape[0] - cut)):

        def normalise(i, carry, base=base):
            here = pl.ds(pl.multiple_of(i * step, step), step)
            there = pl.ds(pl.multiple_of(base + i * step, step), step)
            if n_sources > 1:
                values = [source[there, :].astype(jnp.float32) for source in sources[:3]]
                values.append(sources[3 if base == 0 else 4][here, :].astype(jnp.float32))
            else:
                values = [sources[0][block, there, :].astype(jnp.float32) for block in blocks]
            total = sum(jnp.sum(v * v, axis=1, keepdims=True) for v in values)
            scale = lax.rsqrt(total * (1.0 / (512 * NX)) + epsilon)
            for block, v in zip(blocks, values):
                columns = pl.ds(pl.multiple_of(block * 512, 512), 512)
                scaled = v * scale * gains[index, pl.ds(block, 1), :]
                normed[there, columns] = scaled.astype(jnp.bfloat16)
            return carry

        steps = count // step
        lax.fori_loop(0, steps, normalise, 0, unroll=2 if steps % 2 == 0 else 1)

    for piece, units in zip(pieces, units_of(index, y, z, c, 2 * c - 1)):
        for k, (mat, z_at, y_at) in enumerate(units):
            row = pl.multiple_of(z_at * 256 + y_at * 64, 64)
            weights[mat, pl.ds(row, 64), :] = piece[k]

    rows = normed.shape[0]
    same = same_ref[...]
    same_before, same_after = same[:, 0:1] > 0.5, same[:, 1:2] > 0.5

    def mix(n, carry):
        columns = pl.ds(pl.multiple_of(n * 256, 256), 256)

        def project(mat):
            value = jnp.dot(normed[...], weights[mat, :, columns], preferred_element_type=jnp.float32)
            return value.astype(jnp.bfloat16).astype(jnp.float32)

        mixed = (project(0) * project(1)).astype(jnp.bfloat16).astype(jnp.float32)
        before = pltpu.roll(mixed, 1, 0)
        after = pltpu.roll(mixed, rows - 1, 0)
        convolved = (
            jnp.where(same_before, taps[index, 0:1, columns] * before, 0.0)
            + taps[index, 1:2, columns] * mixed
            + jnp.where(same_after, taps[index, 2:3, columns] * after, 0.0)
        )
        gated[:, columns] = (project(2) * convolved).astype(jnp.bfloat16)
        return carry

    lax.fori_loop(0, 2, mix, 0)

    for place, off in enumerate((0, 1, -1, 2)):
        block = lax.rem(x + off + NX, NX)

        def project_out(n, carry, place=place, block=block):
            value = lax.dot_general(
                gated[...],
                weights[3, pl.ds(pl.multiple_of(block * 512 + n * 256, 256), 256), :],
                (((1,), (1,)), ((), ())),
                preferred_element_type=jnp.float32,
            ).astype(jnp.bfloat16)
            columns = pl.ds(pl.multiple_of(n * 256, 256), 256)
            if place < 3:
                outs[place][:, columns] = value
            else:
                outs[3][:, columns] = value[:cut]
                outs[4][:, columns] = value[cut:]
            return carry

        lax.fori_loop(0, 2, project_out, 0)


def layer(index, cut, sources, gains, same, taps, pieces):
    rows = same.shape[0]
    vmem = pl.BlockSpec(memory_space=pltpu.VMEM)
    return pl.pallas_call(
        functools.partial(layer_kernel, index, cut, len(sources), len(pieces)),
        out_shape=[jax.ShapeDtypeStruct((n, 512), jnp.bfloat16) for n in (rows, rows, rows, cut, rows - cut)],
        in_specs=[vmem] * (len(sources) + 3 + len(pieces)),
        out_specs=[vmem] * 5,
        scratch_shapes=[
            pltpu.VMEM((rows, 2048), jnp.bfloat16),
            pltpu.VMEM((rows, 512), jnp.bfloat16),
            pltpu.VMEM((4, 2048, 512), jnp.bfloat16),
        ],
        compiler_params=pltpu.CompilerParams(vmem_limit_bytes=VMEM_LIMIT << 20),
        cost_estimate=pl.CostEstimate(flops=2 * rows * 2048 * 2048, bytes_accessed=8 << 20, transcendentals=rows),
    )(*sources, gains, same, taps, *pieces)


def per_device(stream, doc_ids, norm_gain, gate_proj, input_gate, value_proj, taps, out_proj):
    c = lax.axis_index("c")
    mats = jnp.stack([input_gate, value_proj, gate_proj, jnp.swapaxes(out_proj, 1, 2)], axis=1)
    chip = lax.all_gather(mats, "c", axis=2, tiled=True)

    ids = jnp.broadcast_to(doc_ids.astype(jnp.bfloat16)[:, None], (doc_ids.shape[0], 128))
    wider = with_edges(jnp.concatenate([stream, ids], axis=1), c)
    rows = wider[:, :512]
    gathered = gather_first(rows)
    me, length = lax.axis_index(SP), doc_ids.shape[0]
    docs = wider[:, 512].astype(jnp.float32)
    place = lax.broadcasted_iota(jnp.int32, (length + 2 * HALO,), 0) + me * length
    docs = jnp.where((place < HALO) | (place >= lax.axis_size(SP) * length + HALO), -1.0, docs)
    equal = (docs[1:] == docs[:-1]).astype(jnp.float32)
    none = jnp.zeros((1,), jnp.float32)
    same = jnp.stack([jnp.concatenate([none, equal]), jnp.concatenate([equal, none])], axis=1)
    gains = norm_gain.reshape(-1, NX, 512)
    pieces = [by_y_then_z(chip[0, :2], c) + by_z_then_y(chip[0, 2:], c), by_y_then_z(chip[1], c)]

    cut = (rows.shape[0] // 32 + 1) * 16
    sources = [gathered]
    for index in range(2):
        parts = layer(index, cut, sources, gains, same, taps, pieces[index])
        rows = scatter_x(rows, *parts)
        if index == 0:
            sources = gather_x(rows, cut)
    return rows[HALO:-HALO]


def solution(mesh):
    split = Mesh(mesh.devices.reshape(NZ, NY, NC, NX), ("z", "y", "c", "x"))
    in_specs = (
        P(SP, "x"),
        P(SP),
        P(),
        P(None, SP, "x"),
        P(None, SP, "x"),
        P(None, SP, "x"),
        P(None, None, "x"),
        P(None, "x", SP),
    )

    return jax.shard_map(per_device, mesh=split, in_specs=in_specs, out_specs=P(SP, "x"), check_vma=False)
```
